32 devices in a mesh: grp: 2 (over x), ep: 16 (over z, y, core).
Axes of the slice: x: 2, y: 2, z: 4, core: 2. Of those that a mesh axis runs over, the one named last changes fastest.
Arguments:
- tokens: bfloat16 [16384, 2048], P(('grp', 'ep')), parts along dimension 0, may hold values from -6 to 6
- norm_gain: float32 [2048], replicated, may hold values from 0.1 to 1.9
- route_ids: int32 [16384, 2], P(('grp', 'ep')), parts along dimension 0, may hold values from 0 to 15, all different within a row; in each aligned block of 512 rows (0 to 511, 512 to 1023, ...) at most 96 rows name the same one
- route_gates: float32 [16384, 2], P(('grp', 'ep')), parts along dimension 0, may hold values from 0.05 to 1
- w_gate: bfloat16 [16, 2048, 1024], P('ep'), may hold values from -0.125 to 0.125
- w_up: bfloat16 [16, 2048, 1024], P('ep'), may hold values from -0.125 to 0.125
- w_down: bfloat16 [16, 1024, 2048], P('ep'), may hold values from -0.1875 to 0.1875
Outputs:
- mixed: bfloat16 [16384, 2048], P(('grp', 'ep')), parts along dimension 0
The draws below stay inside these ranges and needn't reach their ends.
There are 2 independent parts, one for each index of `grp`. The reference program is written for one: setup_inputs(seed, part) draws one part's arguments, and reference() takes and returns one part's arrays. A program takes and returns all parts, laid end to end along the dimension named above; an argument that names none is the same for every part. Nothing has to cross between parts.
Inputs may be any that keep to these rules, and one draw needn't show every extreme that they name: `route_ids`: each row names 2 different experts. Among the rows of one device no expert is named more than 96 times, and in some devices' rows one expert is named exactly 96 times.
All inputs are finite; a program needn't handle non-finite values.
Results may differ from the reference program's by a relative error of at most 0.0071.
Values may be sent and summed in bfloat16 or wider, within the bound.
A program may use at most 128 MiB of HBM per device.

```python
import math
import jax
import jax.numpy as jnp
import numpy as np
from jax import lax

D = 2048
FF = 1024
TOPK = 2
TOK_DEV = 512
EXPERTS = 16
CAP = 96
TOKENS = 8192
N_EP = 16


def steps_of(rng, dims, split, low, top_value):
    level = 1.0
    for axis_at, parts in split:
        draws = jax.random.uniform(jax.random.fold_in(jax.random.fold_in(rng, 6), axis_at), (parts,), jnp.float32, low / len(split), top_value / len(split))
        level = level * jnp.repeat(jnp.exp(draws), dims[axis_at] // parts).reshape((-1,) + (1,) * (len(dims) - 1 - axis_at))
    return level


def shared_out(key, own, number, rows, number_of, top, most, slope):
    sequence = jax.random.permutation(key, number_of)
    packed, common = shares(number_of, rows * top, most, slope, True), shares(number_of, rows * top, most, slope, False)
    places = jnp.arange(number_of)

    def named(lengths, offset_by):
        used = int((lengths > 0).sum())
        fixed = max(1, used // 4)
        shifted = fixed + (places - fixed + offset_by * (used - fixed)) % max(1, number_of - fixed)
        return jnp.zeros((number_of,), jnp.int32).at[sequence[jnp.where(places < fixed, places, shifted)]].set(jnp.asarray(lengths, jnp.int32))

    lengths = jnp.where(number % 4 == 0, named(packed, number // 4), named(common, number - number // 4 - 1))
    mixed = jax.random.permutation(jax.random.fold_in(own, 3), number_of)
    giver, sink = mixed[0:number_of // 2 * 2:2], mixed[1:number_of // 2 * 2:2]
    slack = jnp.minimum(lengths[giver] - 1, most - lengths[sink]) // 2
    slack = jnp.where((giver == sequence[0]) | (sink == sequence[0]) | (lengths[sink] == 0), 0, jnp.maximum(slack, 0))
    shifted = jax.random.randint(jax.random.fold_in(own, 4), (number_of // 2,), 0, 1 << 20) % (slack + 1)
    lengths = lengths.at[giver].add(-shifted).at[sink].add(shifted)
    labels = jnp.searchsorted(jnp.cumsum(lengths), jnp.arange(rows * top), side="right").astype(jnp.int32)
    listing = labels.reshape(top, rows).T
    listing = listing[jax.random.permutation(jax.random.fold_in(own, 1), rows)]
    offset_by = jax.random.randint(jax.random.fold_in(own, 2), (rows, 1), 0, top)
    return jnp.take_along_axis(listing, (jnp.arange(top)[None, :] + offset_by) % top, axis=1)


def shares(number_of, total, most, slope, full):
    weights = [(1 << 20) // math.isqrt(rank ** slope) + 1 for rank in range(1, number_of + 1)]
    largest = most if full else min(most, max(-(-total // number_of), total * weights[0] // sum(weights)))
    least = 1 if total - largest >= number_of - 1 else 0
    counts, rest = [largest] + [least] * (number_of - 1), total - largest - least * (number_of - 1)
    while rest > 0:
        movable = [i for i in range(1, number_of) if counts[i] < largest] or [i for i in range(1, number_of) if counts[i] < most]
        mass, remaining = sum([weights[i] for i in movable]), rest
        for i in movable:
            extra = min(most - counts[i], max(1, remaining * weights[i] // mass), rest)
            counts[i] = counts[i] + extra
            rest = rest - extra
    return np.array(counts)


def scatter_about(own_key, shape, spread, limit, shards=(), held_as=jnp.bfloat16):
    array = jax.random.normal(own_key, shape, jnp.float32) * spread
    if len(shards) > 0:
        array = steps_of(own_key, shape, shards, -0.22, 0.18) * array
    return jnp.clip(array, min=-limit, max=limit).astype(held_as)


def setup_inputs(seed: int = 0, part: int = 0) -> dict:
    streams_of = jax.random.split(jax.random.key(seed), 8)
    part_splits = jax.random.split(jax.random.fold_in(streams_of[7], part), 8)
    tokens = scatter_about(part_splits[0], (TOKENS, D), 1.0, 6.0, ((0, 16),))
    norm_gain = jnp.clip(1.0 + 0.18 * jax.random.normal(streams_of[1], (D,), jnp.float32), 0.1, 1.9)
    route_ids_keys = jax.random.split(jax.random.fold_in(part_splits[2], 1), TOKENS // TOK_DEV)
    route_ids_turns = jax.random.permutation(jax.random.fold_in(part_splits[2], 3), TOKENS // TOK_DEV)
    route_ids = jax.vmap(lambda own, number: shared_out(jax.random.fold_in(part_splits[2], 2), own, number, TOK_DEV, EXPERTS, TOPK, CAP, 2))(route_ids_keys, route_ids_turns).reshape((TOKENS, TOPK))
    route_gates = jnp.clip(0.05 + 0.95 * jax.random.uniform(part_splits[3], (TOKENS, TOPK), jnp.float32) ** steps_of(part_splits[3], (TOKENS, TOPK), ((0, 16),), -0.2, 0.2), 0.05, 1.0)
    w_gate = scatter_about(streams_of[4], (EXPERTS, D, FF), D ** -0.5, 0.125, ((0, 16),))
    w_up = scatter_about(streams_of[5], (EXPERTS, D, FF), D ** -0.5, 0.125, ((0, 16),))
    w_down = scatter_about(streams_of[6], (EXPERTS, FF, D), FF ** -0.5, 0.1875, ((0, 16),))
    return dict(tokens=tokens, norm_gain=norm_gain, route_ids=route_ids, route_gates=route_gates, w_gate=w_gate, w_up=w_up, w_down=w_down)


EPS = 1e-06

def reference(tokens, norm_gain, route_ids, route_gates, w_gate, w_up, w_down):
    floats = tokens.astype(jnp.float32)
    scale = lax.rsqrt(lax.optimization_barrier(jnp.mean(floats * floats, axis=-1, keepdims=True)) + EPS)
    normed = (floats * scale * norm_gain).astype(jnp.bfloat16)
    weights = route_gates / lax.optimization_barrier(jnp.sum(route_gates, axis=-1, keepdims=True))
    count = TOKENS * TOPK
    flat_ids = route_ids.reshape(-1)
    flat_weights = weights.reshape(-1)
    most = N_EP * CAP

    def one_expert(carry, inputs):
        expert, gate_mat, up_mat, down_mat = inputs
        picked = jnp.nonzero(flat_ids == expert, size=most, fill_value=count)[0].astype(jnp.int32)
        live = picked < count
        pairs = jnp.minimum(picked, count - 1)
        rows = pairs // TOPK
        chosen = normed[rows]
        gate_pre = jnp.dot(chosen, gate_mat, preferred_element_type=jnp.float32)
        up_pre = jnp.dot(chosen, up_mat, preferred_element_type=jnp.float32)
        hidden = (jax.nn.silu(gate_pre) * up_pre).astype(jnp.bfloat16)
        result = jnp.dot(hidden, down_mat, preferred_element_type=jnp.float32).astype(jnp.bfloat16)
        factor = jnp.where(live, flat_weights[pairs], jnp.zeros_like(flat_weights[pairs]))
        return (carry.at[rows].add(result.astype(jnp.float32) * factor[:, None]), None)
    start = jnp.zeros((TOKENS, D), jnp.float32)
    total, _ = lax.scan(one_expert, start, (jnp.arange(EXPERTS, dtype=jnp.int32), w_gate, w_up, w_down))
    return total.astype(jnp.bfloat16)
```

```python
import jax
import jax.numpy as jnp
from jax import lax
from jax.sharding import PartitionSpec as P

EPS = 1e-06
CHUNKS = 2


def rms_norm(tokens, norm_gain):
    floats = tokens.astype(jnp.float32)
    scale = lax.rsqrt(jnp.mean(floats * floats, axis=-1, keepdims=True) + EPS)
    return (floats * scale * norm_gain).astype(jnp.bfloat16)


def slot_index(route_ids, experts, capacity):
    rows, top = route_ids.shape
    hit = [route_ids[:, k : k + 1] == jnp.arange(experts, dtype=jnp.int32)[None, :] for k in range(top)]
    named = sum(h.astype(jnp.float32) for h in hit)
    before = (jnp.arange(rows)[:, None] > jnp.arange(rows)[None, :]).astype(jnp.bfloat16)
    ranked = jnp.dot(before, named.astype(jnp.bfloat16), preferred_element_type=jnp.float32)
    base = ranked + jnp.arange(experts, dtype=jnp.float32)[None, :] * capacity
    return jnp.stack([jnp.sum(jnp.where(h, base, 0.0), axis=1) for h in hit])


def dispatch_matrix(places, first, count):
    slots = first + jnp.arange(count, dtype=jnp.int32)[:, None]
    hit = places[0][None, :] == slots
    for k in range(1, places.shape[0]):
        hit = hit | (places[k][None, :] == slots)
    return hit.astype(jnp.bfloat16)


def combine_matrix(places, weights, first, count):
    slots = first + jnp.arange(count, dtype=jnp.int32)[None, :]
    total = sum(
        jnp.where(places[k][:, None] == slots, weights[k][:, None], 0.0) for k in range(places.shape[0])
    )
    high = total.astype(jnp.bfloat16)
    low = (total - high.astype(jnp.float32)).astype(jnp.bfloat16)
    return high, low


def dot32(a, b):
    return jnp.dot(a, b, preferred_element_type=jnp.float32)


def hidden_of(rows, w_gate, w_up):
    gate_pre = dot32(rows, w_gate)
    up_pre = dot32(rows, w_up)
    return (jax.nn.silu(gate_pre) * up_pre).astype(jnp.bfloat16)


def body(tokens, norm_gain, route_ids, route_gates, w_gate, w_up, w_down):
    tok_rows, width = tokens.shape
    top_count = route_ids.shape[1]
    devices = lax.axis_size("ep")
    local_experts = w_gate.shape[0]
    experts = local_experts * devices
    capacity = 3 * tok_rows * top_count // (2 * experts)
    half = devices // 2
    me = lax.axis_index("ep")
    side = me // half
    groups = [list(range(half)), list(range(half, devices))]
    across = [(i, (i + half) % devices) for i in range(devices)]
    block = local_experts * capacity
    count = half * block
    first = side * count
    step = width // CHUNKS

    def cross(value):
        return lax.ppermute(value, "ep", across)

    def exchange(value):
        return lax.all_to_all(value, "ep", 0, 0, axis_index_groups=groups, tiled=True)

    normed = rms_norm(tokens, norm_gain)
    far = [cross(normed[:, c * step : (c + 1) * step]) for c in range(CHUNKS)]
    weights = (route_gates / jnp.sum(route_gates, axis=1, keepdims=True)).T
    places = slot_index(route_ids, experts, capacity)
    table = cross(jnp.concatenate([places, weights]))
    places, far_places = places.astype(jnp.int32), table[:top_count].astype(jnp.int32)
    far_weights = table[top_count:]

    def send(matrix, parts):
        got = [exchange(dot32(matrix, part).astype(jnp.bfloat16)) for part in parts]
        got = got[0] if len(got) == 1 else jnp.concatenate(got, axis=1)
        return got.reshape(half, local_experts, capacity, width)

    def finish(arrived):
        mids = []
        for j in range(local_experts):
            rows = arrived[:, j].reshape(half * capacity, width)
            mids.append(hidden_of(rows, w_gate[j], w_up[j]))

        def out(c):
            ends = [
                dot32(mids[j], w_down[j, :, c * step : (c + 1) * step])
                .astype(jnp.bfloat16)
                .reshape(half, 1, capacity, step)
                for j in range(local_experts)
            ]
            ends = ends[0] if local_experts == 1 else jnp.concatenate(ends, axis=1)
            return exchange(ends.reshape(count, step))

        return out

    own_out = finish(send(dispatch_matrix(places, first, count), [normed]))
    far_out = finish(send(dispatch_matrix(far_places, first, count), far))
    far_high, far_low = combine_matrix(far_places, far_weights, first, count)
    high, low = combine_matrix(places, weights, first, count)
    partial = []
    for c in range(CHUNKS):
        back = far_out(c)
        partial.append(cross((dot32(far_high, back) + dot32(far_low, back)).astype(jnp.bfloat16)))
    mixed = []
    for c in range(CHUNKS):
        back = own_out(c)
        total = dot32(high, back) + dot32(low, back) + partial[c].astype(jnp.float32)
        mixed.append(total.astype(jnp.bfloat16))
    return jnp.concatenate(mixed, axis=1)


def solution(mesh):
    placed = (
        P(("grp", "ep"), None),
        P(),
        P(("grp", "ep"), None),
        P(("grp", "ep"), None),
        P("ep", None, None),
        P("ep", None, None),
        P("ep", None, None),
    )
    return jax.shard_map(
        body, mesh=mesh, in_specs=placed, out_specs=P(("grp", "ep"), None), check_vma=False
    )
```

```python
import functools

import jax
import jax.numpy as jnp
from jax import lax
from jax.experimental import pallas as pl
from jax.experimental.pallas import tpu as pltpu
from jax.sharding import PartitionSpec as P

EPS = 1e-06
CHUNKS = 4
TILE = 256
VMEM_BYTES = 66000000


def rms_norm(tokens, norm_gain):
    floats = tokens.astype(jnp.float32)
    scale = lax.rsqrt(jnp.mean(floats * floats, axis=-1, keepdims=True) + EPS)
    return (floats * scale * norm_gain).astype(jnp.bfloat16)


def slot_index(route_ids, experts, capacity):
    rows, top = route_ids.shape
    hit = [route_ids[:, k : k + 1] == jnp.arange(experts, dtype=jnp.int32)[None, :] for k in range(top)]
    named = sum(h.astype(jnp.float32) for h in hit)
    before = (jnp.arange(rows)[:, None] > jnp.arange(rows)[None, :]).astype(jnp.bfloat16)
    ranked = jnp.dot(before, named.astype(jnp.bfloat16), preferred_element_type=jnp.float32)
    base = ranked + jnp.arange(experts, dtype=jnp.float32)[None, :] * capacity
    return jnp.stack([jnp.sum(jnp.where(h, base, 0.0), axis=1) for h in hit])


def dot32(a, b):
    return jnp.dot(a, b, preferred_element_type=jnp.float32)


def kernel(
    devices, capacity, top,
    normed, table, gate_hbm, up_hbm, down_hbm,
    mixed,
    far, far_table, takes, highs, lows, packed, arrived, hidden, w_gate, w_up, w_down,
    outs, backs, partial, partial_in,
    weight_sems, table_sems, far_send, far_recv, own_sems, self_sems, go_send, go_recv,
    back_send, back_recv, part_send, part_recv,
):
    half = devices // 2
    chunks, rows, step = normed.shape
    count = half * capacity
    ff = w_gate.shape[1]
    me = lax.axis_index("ep")
    q = me % half
    base = me - q
    partner = (me + half) % devices
    first = base * capacity

    def peer_at(i):
        off = (half // 2 + i) % half + (half // 2 + i) // half
        return (q + off) % half

    barrier = pltpu.get_barrier_semaphore()

    def greet(i, carry):
        pl.semaphore_signal(barrier, inc=1, device_id={"ep": base + peer_at(i)})
        return carry

    lax.fori_loop(0, half - 1, greet, 0)
    pl.semaphore_signal(barrier, inc=1, device_id={"ep": partner})

    loads = [
        pltpu.make_async_copy(gate_hbm.at[0], w_gate, weight_sems.at[0]),
        pltpu.make_async_copy(up_hbm.at[0], w_up, weight_sems.at[1]),
        pltpu.make_async_copy(down_hbm.at[0], w_down, weight_sems.at[2]),
    ]
    pl.semaphore_wait(barrier, half)

    def remote(src, dst, send, recv, device):
        return pltpu.make_async_remote_copy(
            src_ref=src, dst_ref=dst, send_sem=send, recv_sem=recv, device_id={"ep": device}
        )

    def table_copy():
        return remote(table, far_table, table_sems.at[0], table_sems.at[1], partner)

    def far_copy(c):
        return remote(normed.at[c], far.at[c], far_send.at[c], far_recv.at[c], partner)

    def part_copy(c):
        return remote(partial.at[c], partial_in.at[c], part_send.at[c], part_recv.at[c], partner)

    def span(j):
        return pl.ds(pl.multiple_of(j * capacity, 16), capacity)

    def go_copy(s, c, peer, slot):
        return remote(
            packed.at[s, c, span(peer)], arrived.at[s, c, span(q)],
            go_send.at[s, c, slot], go_recv.at[s, c, q], base + peer,
        )

    def back_copy(s, c, peer, slot):
        return remote(
            outs.at[s, c, span(peer)], backs.at[s, c, span(q)],
            back_send.at[s, c, slot], back_recv.at[s, c, q], base + peer,
        )

    def go_arrival(s, c, peer):
        return remote(
            packed.at[s, c, span(peer)], arrived.at[s, c, span(peer)],
            go_send.at[s, c, 0], go_recv.at[s, c, peer], base + peer,
        )

    def back_arrival(s, c, peer):
        return remote(
            outs.at[s, c, span(peer)], backs.at[s, c, span(peer)],
            back_send.at[s, c, 0], back_recv.at[s, c, peer], base + peer,
        )

    def go_self(s, c):
        return pltpu.make_async_copy(packed.at[s, c, span(q)], arrived.at[s, c, span(q)], own_sems.at[s, c])

    def back_self(s, c):
        return pltpu.make_async_copy(outs.at[s, c, span(q)], backs.at[s, c, span(q)], self_sems.at[s, c])

    def each_peer(act):
        def one(i, carry):
            act(peer_at(i), i)
            return carry

        lax.fori_loop(0, half - 1, one, 0)

    def matrices(s, source):
        width = 128

        def one(i, carry):
            at = pl.multiple_of(i * width, width)
            slots = (first + at + lax.broadcasted_iota(jnp.int32, (width, rows), 0)).astype(jnp.float32)
            taken = jnp.zeros((width, rows), jnp.float32)
            total = jnp.zeros((width, rows), jnp.float32)
            for k in range(top):
                hit = source[k : k + 1, :] == slots
                taken = taken + jnp.where(hit, 1.0, 0.0)
                total = total + jnp.where(hit, source[top + k : top + k + 1, :], 0.0)
            takes[s, pl.ds(at, width), :] = taken.astype(jnp.bfloat16)
            turned = total.T
            high = turned.astype(jnp.bfloat16)
            highs[s, :, pl.ds(at, width)] = high
            lows[s, :, pl.ds(at, width)] = (turned - high.astype(jnp.float32)).astype(jnp.bfloat16)
            return carry

        lax.fori_loop(0, count // width, one, 0)

    def tiles(act):
        def one(i, carry):
            act(pl.ds(pl.multiple_of(i * TILE, TILE), TILE))
            return carry

        lax.fori_loop(0, step // TILE, one, 0)

    def pack(s, c, source):
        def one(cols):
            packed[s, c, :, cols] = dot32(takes[s], source[c, :, cols]).astype(jnp.bfloat16)

        tiles(one)
        each_peer(lambda peer, i: go_copy(s, c, peer, i).start())
        go_self(s, c).start()

    def wait_go(s, c):
        each_peer(lambda peer, i: go_arrival(s, c, peer).wait_recv())
        go_self(s, c).wait()

    def expert_hidden(s):
        def one(i, carry):
            cols = pl.ds(pl.multiple_of(i * TILE, TILE), TILE)
            gate_pre = dot32(arrived[s, 0], w_gate[0:step, cols])
            up_pre = dot32(arrived[s, 0], w_up[0:step, cols])
            for c in range(1, chunks):
                gate_pre += dot32(arrived[s, c], w_gate[c * step : (c + 1) * step, cols])
                up_pre += dot32(arrived[s, c], w_up[c * step : (c + 1) * step, cols])
            hidden[s, :, cols] = (gate_pre / (1.0 + jnp.exp(-gate_pre)) * up_pre).astype(jnp.bfloat16)
            return carry

        lax.fori_loop(0, ff // TILE, one, 0)

    def expert_out(s, c):
        def one(i, carry):
            at = pl.multiple_of(i * TILE, TILE)
            cols = pl.ds(pl.multiple_of(c * step + at, TILE), TILE)
            outs[s, c, :, pl.ds(at, TILE)] = dot32(hidden[s], w_down[:, cols]).astype(jnp.bfloat16)
            return carry

        lax.fori_loop(0, step // TILE, one, 0)

    def send_back(s, c):
        each_peer(lambda peer, i: back_copy(s, c, peer, i).start())
        back_self(s, c).start()

    def wait_back(s, c):
        each_peer(lambda peer, i: back_arrival(s, c, peer).wait_recv())
        back_self(s, c).wait()

    table_copy().start()
    far_copy(0).start()
    for load in loads:
        load.start()
    matrices(0, table)
    for c in range(chunks):
        pack(0, c, normed)
        if c + 1 < chunks:
            far_copy(c + 1).start()
    table_copy().wait()
    matrices(1, far_table)
    for c in range(chunks):
        far_copy(c).wait_recv()
        pack(1, c, far)
        if c == chunks - 2:
            for s_c in range(chunks):
                wait_go(0, s_c)
            for load in loads:
                load.wait()
            expert_hidden(0)
            for d in range(chunks):
                expert_out(0, d)
    for c in range(chunks):
        wait_go(1, c)
    expert_hidden(1)
    for c in range(chunks):
        expert_out(1, c)
        send_back(1, c)
    for c in range(chunks):
        wait_back(1, c)

        def merge(cols):
            back = backs[1, c, :, cols]
            partial[c, :, cols] = (dot32(highs[1], back) + dot32(lows[1], back)).astype(jnp.bfloat16)

        tiles(merge)
        part_copy(c).start()
        send_back(0, c)
    for c in range(chunks):
        wait_back(0, c)
        part_copy(c).wait_recv()

        def close(i, carry):
            at = pl.multiple_of(i * TILE, TILE)
            cols = pl.ds(at, TILE)
            back = backs[0, c, :, cols]
            total = dot32(highs[0], back) + dot32(lows[0], back) + partial_in[c, :, cols].astype(jnp.float32)
            mixed[:, pl.ds(pl.multiple_of(c * step + at, TILE), TILE)] = total.astype(jnp.bfloat16)
            return carry

        lax.fori_loop(0, step // TILE, close, 0)
    for c in range(chunks):
        far_copy(c).wait_send()
        part_copy(c).wait_send()
        for s in range(2):
            each_peer(lambda peer, i: go_copy(s, c, peer, i).wait_send())
            each_peer(lambda peer, i: back_copy(s, c, peer, i).wait_send())


def body(tokens, norm_gain, route_ids, route_gates, w_gate, w_up, w_down):
    rows, width = tokens.shape
    top = route_ids.shape[1]
    devices = lax.axis_size("ep")
    experts = devices
    ff = w_gate.shape[2]
    capacity = 3 * rows * top // (2 * experts)
    half = devices // 2
    count = half * capacity
    step = width // CHUNKS
    normed = rms_norm(tokens, norm_gain).reshape(rows, CHUNKS, step).transpose(1, 0, 2)
    weights = (route_gates / jnp.sum(route_gates, axis=1, keepdims=True)).T
    table = jnp.concatenate([slot_index(route_ids, experts, capacity), weights])
    vmem = pl.BlockSpec(memory_space=pltpu.VMEM)
    hbm = pl.BlockSpec(memory_space=pl.ANY)
    bf16 = jnp.bfloat16
    dma = pltpu.SemaphoreType.DMA
    return pl.pallas_call(
        functools.partial(kernel, devices, capacity, top),
        out_shape=jax.ShapeDtypeStruct((rows, width), bf16),
        in_specs=[vmem, vmem, hbm, hbm, hbm],
        out_specs=vmem,
        scratch_shapes=[
            pltpu.VMEM((CHUNKS, rows, step), bf16),
            pltpu.VMEM(table.shape, jnp.float32),
            pltpu.VMEM((2, count, rows), bf16),
            pltpu.VMEM((2, rows, count), bf16),
            pltpu.VMEM((2, rows, count), bf16),
            pltpu.VMEM((2, CHUNKS, count, step), bf16),
            pltpu.VMEM((2, CHUNKS, count, step), bf16),
            pltpu.VMEM((2, count, ff), bf16),
            pltpu.VMEM((width, ff), bf16),
            pltpu.VMEM((width, ff), bf16),
            pltpu.VMEM((ff, width), bf16),
            pltpu.VMEM((2, CHUNKS, count, step), bf16),
            pltpu.VMEM((2, CHUNKS, count, step), bf16),
            pltpu.VMEM((CHUNKS, rows, step), bf16),
            pltpu.VMEM((CHUNKS, rows, step), bf16),
            dma((3,)),
            dma((2,)),
            dma((CHUNKS,)),
            dma((CHUNKS,)),
            dma((2, CHUNKS)),
            dma((2, CHUNKS)),
            dma((2, CHUNKS, half)),
            dma((2, CHUNKS, half)),
            dma((2, CHUNKS, half)),
            dma((2, CHUNKS, half)),
            dma((CHUNKS,)),
            dma((CHUNKS,)),
        ],
        compiler_params=pltpu.CompilerParams(
            collective_id=0, has_side_effects=True, vmem_limit_bytes=VMEM_BYTES
        ),
    )(normed, table, w_gate, w_up, w_down)


def solution(mesh):
    placed = (
        P(("grp", "ep"), None),
        P(),
        P(("grp", "ep"), None),
        P(("grp", "ep"), None),
        P("ep", None, None),
        P("ep", None, None),
        P("ep", None, None),
    )
    return jax.shard_map(
        body, mesh=mesh, in_specs=placed, out_specs=P(("grp", "ep"), None), check_vma=False
    )
```

```python
import functools

import jax
import jax.numpy as jnp
from jax import lax
from jax.experimental import pallas as pl
from jax.experimental.pallas import tpu as pltpu
from jax.sharding import PartitionSpec as P

EPS = 1e-06
CHUNKS = 4
TILE = 256
VMEM_BYTES = 67000000


def slot_index(route_ids, experts, capacity):
    rows, top = route_ids.shape
    hit = [route_ids[:, k : k + 1] == jnp.arange(experts, dtype=jnp.int32)[None, :] for k in range(top)]
    named = sum(h.astype(jnp.float32) for h in hit)
    before = (jnp.arange(rows)[:, None] > jnp.arange(rows)[None, :]).astype(jnp.bfloat16)
    ranked = jnp.dot(before, named.astype(jnp.bfloat16), preferred_element_type=jnp.float32)
    base = ranked + jnp.arange(experts, dtype=jnp.float32)[None, :] * capacity
    return jnp.stack([jnp.sum(jnp.where(h, base, 0.0), axis=1) for h in hit])


def dot32(a, b):
    return jnp.dot(a, b, preferred_element_type=jnp.float32)


def kernel(
    devices, capacity, top,
    tokens_hbm, gain, table, gate_hbm, up_hbm, down_hbm,
    mixed,
    normed, near, far_in, far_out, tables, takes, highs, packed, packed_o, arrived, hidden,
    w_gate, w_up, w_down, backs, backs_o, sum_own, sum_near,
    load_sems, table_send, table_recv, near_send, near_recv, fin_send, fin_recv, fout_send, fout_recv,
    go_send, go_recv, goo_send, back_send, back_recv, backo_recv, self_go, self_back,
    own_send, own_recv, rel_send, rel_recv, up_send, up_recv,
):
    half, quarter = devices // 2, devices // 4
    chunks, rows, step = normed.shape
    count = half * capacity
    ff = w_gate.shape[1]
    width = chunks * step
    me = lax.axis_index("ep")
    place, p = me // quarter, me % quarter
    side = me // half
    q = me % half
    base = side * half
    plane = place * quarter
    inner_plane = (1 + side) * quarter
    inner_dev = inner_plane + p
    outer_dev = 3 * side * quarter + p
    far_dev = (2 - side) * quarter + p
    is_inner = place == 1 + side
    is_outer = place != 1 + side
    outer_plane_q = (1 - (place - 2 * side)) * quarter

    def peer_at(i):
        off = (half // 2 + i) % half + (half // 2 + i) // half
        return (q + off) % half

    barrier = pltpu.get_barrier_semaphore()

    def greet(i, carry):
        pl.semaphore_signal(barrier, inc=1, device_id={"ep": base + peer_at(i)})
        return carry

    loads = [
        pltpu.make_async_copy(gate_hbm.at[0], w_gate, load_sems.at[0]),
        pltpu.make_async_copy(up_hbm.at[0], w_up, load_sems.at[1]),
        pltpu.make_async_copy(down_hbm.at[0], w_down, load_sems.at[2]),
    ]
    token_load = pltpu.make_async_copy(tokens_hbm, mixed, load_sems.at[3])
    token_load.start()
    lax.fori_loop(0, half - 1, greet, 0)

    @pl.when(is_inner)
    def _():
        pl.semaphore_signal(barrier, inc=1, device_id={"ep": far_dev})

    token_load.wait()
    for load in loads:
        load.start()

    def norm(i, carry):
        at = pl.ds(pl.multiple_of(i * 64, 64), 64)
        floats = mixed[at, :].astype(jnp.float32)
        scale = lax.rsqrt(jnp.mean(floats * floats, axis=-1, keepdims=True) + EPS)
        value = (floats * scale * gain[...]).astype(jnp.bfloat16)
        for c in range(chunks):
            normed[c, at, :] = value[:, c * step : (c + 1) * step]
        return carry

    lax.fori_loop(0, rows // 64, norm, 0)

    @pl.when(is_inner)
    def _():
        pl.semaphore_wait(barrier, half)

    @pl.when(is_outer)
    def _():
        pl.semaphore_wait(barrier, half - 1)

    def remote(src, dst, send, recv, device):
        return pltpu.make_async_remote_copy(
            src_ref=src, dst_ref=dst, send_sem=send, recv_sem=recv, device_id={"ep": device}
        )

    def span(j):
        return pl.ds(pl.multiple_of(j * capacity, 16), capacity)

    def table_to(k, source, device):
        return remote(source, tables.at[k], table_send.at[k], table_recv.at[k], device)

    def near_copy(c):
        return remote(normed.at[c], near.at[c], near_send.at[c], near_recv.at[c], inner_dev)

    def fin_copy(c):
        return remote(normed.at[c], far_in.at[c], fin_send.at[c], fin_recv.at[c], far_dev)

    def fout_copy(c):
        return remote(near.at[c], far_out.at[c], fout_send.at[c], fout_recv.at[c], far_dev)

    def own_sum(c):
        return remote(far_in.at[c], sum_own.at[c], own_send.at[c], own_recv.at[c], far_dev)

    def near_sum(c):
        return remote(far_out.at[c], sum_near.at[c], rel_send.at[c], rel_recv.at[c], far_dev)

    def up_copy(c):
        return remote(near.at[c], near.at[c], up_send.at[c], up_recv.at[c], outer_dev)

    def go_copy(k, c, peer, slot):
        return remote(
            packed.at[max(k - 1, 0), c, span(peer)], arrived.at[k, c, span(p)],
            go_send.at[max(k - 1, 0), c, slot], go_recv.at[k, c, p], base + peer,
        )

    def goo_copy(c, other, slot):
        return remote(
            packed_o.at[c, span(other)], arrived.at[1, c, span(p)],
            goo_send.at[c, slot], go_recv.at[1, c, p], plane + other,
        )

    def arrival(k, c, other, device):
        return remote(
            packed_o.at[c, span(other)], arrived.at[k, c, span(other)],
            goo_send.at[c, 0], go_recv.at[k, c, other], device,
        )

    def back_copy(k, c, other, slot):
        if k == 1:
            return remote(
                arrived.at[1, c, span(other)], backs_o.at[c, span(p)],
                back_send.at[1, c, slot], backo_recv.at[c, p], plane + other,
            )
        return remote(
            arrived.at[k, c, span(other)], backs.at[max(k - 1, 0), c, span(q)],
            back_send.at[k, c, slot], back_recv.at[max(k - 1, 0), c, q], inner_plane + other,
        )

    def back_arrival(k, c, peer):
        return remote(
            arrived.at[k, c, span(0)], backs.at[max(k - 1, 0), c, span(peer)],
            back_send.at[k, c, 0], back_recv.at[max(k - 1, 0), c, peer], base + peer,
        )

    def backo_arrival(c, other):
        return remote(
            arrived.at[1, c, span(0)], backs_o.at[c, span(other)],
            back_send.at[1, c, 0], backo_recv.at[c, other], plane + other,
        )

    def go_self(k, c):
        src = packed_o.at[c, span(p)] if k == 1 else packed.at[max(k - 1, 0), c, span(q)]
        return pltpu.make_async_copy(src, arrived.at[k, c, span(p)], self_go.at[k, c])

    def back_self(k, c):
        dst = backs_o.at[c, span(p)] if k == 1 else backs.at[max(k - 1, 0), c, span(q)]
        return pltpu.make_async_copy(arrived.at[k, c, span(p)], dst, self_back.at[k, c])

    def loop(number, act):
        def one(i, carry):
            act(i)
            return carry

        lax.fori_loop(0, number, one, 0)

    def each_peer(act):
        loop(half - 1, lambda i: act(peer_at(i), i))

    def each_near(act):
        loop(quarter - 1, lambda i: act((p + 1 + i) % quarter, i))

    def each_all(act):
        loop(quarter, lambda i: act((p + i) % quarter, i))

    def matrices(k, source, first, number):
        lanes = 128

        def one(i):
            at = pl.multiple_of(i * lanes, lanes)
            slots = (first + at + lax.broadcasted_iota(jnp.int32, (lanes, rows), 0)).astype(jnp.float32)
            taken = jnp.zeros((lanes, rows), jnp.float32)
            total = jnp.zeros((lanes, rows), jnp.float32)
            for t in range(top):
                hit = source[t : t + 1, :] == slots
                taken = taken + jnp.where(hit, 1.0, 0.0)
                total = total + jnp.where(hit, source[top + t : top + t + 1, :], 0.0)
            takes[k, pl.ds(at, lanes), :] = taken.astype(jnp.bfloat16)
            highs[k, :, pl.ds(at, lanes)] = total.T.astype(jnp.bfloat16)

        loop(number // lanes, one)

    def tiles(act):
        loop(step // TILE, lambda i: act(pl.ds(pl.multiple_of(i * TILE, TILE), TILE)))

    def pack(k, c, source):
        def one(cols):
            packed[max(k - 1, 0), c, :, cols] = dot32(takes[k], source[c, :, cols]).astype(jnp.bfloat16)

        tiles(one)
        each_peer(lambda peer, i: go_copy(k, c, peer, i).start())
        go_self(k, c).start()

    def pack_o(c, source):
        def one(cols):
            packed_o[c, :, cols] = dot32(takes[1, : count // 2], source[c, :, cols]).astype(jnp.bfloat16)

        tiles(one)
        each_near(lambda other, i: goo_copy(c, other, i).start())
        go_self(1, c).start()

    def expert(k, inner):
        for c in range(chunks):
            if k == 1:
                each_near(lambda other, i: arrival(1, c, other, plane + other).wait_recv())
            elif inner:
                each_near(lambda other, i: arrival(k, c, other, inner_plane + other).wait_recv())
            else:
                each_all(lambda other, i: arrival(k, c, other, inner_plane + other).wait_recv())
            if inner or k == 1:
                go_self(k, c).wait()

        def one(i):
            cols = pl.ds(pl.multiple_of(i * TILE, TILE), TILE)
            gate_pre = dot32(arrived[k, 0], w_gate[0:step, cols])
            up_pre = dot32(arrived[k, 0], w_up[0:step, cols])
            for c in range(1, chunks):
                gate_pre += dot32(arrived[k, c], w_gate[c * step : (c + 1) * step, cols])
                up_pre += dot32(arrived[k, c], w_up[c * step : (c + 1) * step, cols])
            hidden[:, cols] = (gate_pre / (1.0 + jnp.exp(-gate_pre)) * up_pre).astype(jnp.bfloat16)

        loop(ff // TILE, one)
        for c in range(chunks):

            def out(i):
                at = pl.multiple_of(i * TILE, TILE)
                cols = pl.ds(pl.multiple_of(c * step + at, TILE), TILE)
                arrived[k, c, :, pl.ds(at, TILE)] = dot32(hidden[...], w_down[:, cols]).astype(jnp.bfloat16)

            loop(step // TILE, out)
            if inner or k == 1:
                each_near(lambda other, i: back_copy(k, c, other, i).start())
                back_self(k, c).start()
            else:
                each_all(lambda other, i: back_copy(k, c, other, i).start())

    def wait_back(k, c):
        each_peer(lambda peer, i: back_arrival(k, c, peer).wait_recv())
        back_self(k, c).wait()

    def wait_backo(c):
        each_near(lambda other, i: backo_arrival(c, other).wait_recv())
        back_self(1, c).wait()

    def combine(k, c, cols):
        return dot32(highs[k], backs[max(k - 1, 0), c, :, cols])

    def combine_o(c, cols):
        return dot32(highs[1, :, : count // 2], backs_o[c, :, cols])

    def out_cols(c, i):
        return pl.ds(pl.multiple_of(c * step + i * TILE, TILE), TILE)

    def in_cols(i):
        return pl.ds(pl.multiple_of(i * TILE, TILE), TILE)

    def wait_loads():
        for load in loads:
            load.wait()

    @pl.when(is_inner)
    def _():
        first = base * capacity
        table_to(2, table, far_dev).start()
        fin_copy(0).start()
        fin_copy(1).start()
        matrices(0, table, first, count)
        for c in range(chunks):
            pack(0, c, normed)
        table_to(1, table, inner_dev).wait_recv()
        table_to(3, tables.at[1], far_dev).start()
        matrices(1, tables.at[1], plane * capacity, count // 2)
        table_to(2, table, far_dev).wait_recv()
        matrices(2, tables.at[2], first, count)

        def relay(c):
            near_copy(c).wait_recv()
            fout_copy(c).start()
            pack_o(c, near)

        def take_in(c):
            fin_copy(c).wait_recv()
            pack(2, c, far_in)

        def take_out(c):
            fout_copy(c).wait_recv()
            pack(3, c, far_out)

        relay(0)
        take_in(0)
        table_to(3, tables.at[1], far_dev).wait_recv()
        matrices(3, tables.at[3], first, count)
        relay(1)
        take_in(1)
        relay(2)
        take_out(0)
        relay(3)
        for c in range(2, chunks):
            fin_copy(c).start()
        wait_loads()
        take_out(1)
        expert(0, True)
        take_out(2)
        expert(1, True)
        take_out(3)
        for c in range(2, chunks):
            take_in(c)
        expert(3, True)
        expert(2, True)

        for c in range(chunks):
            wait_back(3, c)

            def merge_out(cols):
                far_out[c, :, cols] = combine(3, c, cols).astype(jnp.bfloat16)

            tiles(merge_out)
            near_sum(c).start()
        for c in range(chunks):
            wait_back(2, c)

            def merge_in(cols):
                far_in[c, :, cols] = combine(2, c, cols).astype(jnp.bfloat16)

            tiles(merge_in)
            own_sum(c).start()
            wait_backo(c)
            near_sum(c).wait_recv()
            fout_copy(c).wait_send()

            def rise(cols):
                total = combine_o(c, cols) + sum_near[c, :, cols].astype(jnp.float32)
                near[c, :, cols] = total.astype(jnp.bfloat16)

            tiles(rise)
            up_copy(c).start()
        for c in range(chunks):
            wait_back(0, c)
            own_sum(c).wait_recv()

            def close(i):
                total = combine(0, c, in_cols(i)) + sum_own[c, :, in_cols(i)].astype(jnp.float32)
                mixed[:, out_cols(c, i)] = total.astype(jnp.bfloat16)

            loop(step // TILE, close)
        table_to(2, table, far_dev).wait_send()
        table_to(3, tables.at[1], far_dev).wait_send()
        for c in range(chunks):
            fin_copy(c).wait_send()
            near_sum(c).wait_send()
            own_sum(c).wait_send()
            up_copy(c).wait_send()
            each_near(lambda other, i: goo_copy(c, other, i).wait_send())
            for k in (0, 2, 3):
                each_peer(lambda peer, i: go_copy(k, c, peer, i).wait_send())
            for k in range(4):
                each_near(lambda other, i: back_copy(k, c, other, i).wait_send())

    @pl.when(is_outer)
    def _():
        table_to(1, table, inner_dev).start()
        for c in range(chunks):
            near_copy(c).start()
        matrices(1, table, plane * capacity, count // 2)
        for c in range(chunks):
            pack_o(c, normed)
        wait_loads()
        expert(1, False)
        expert(0, False)
        expert(3, False)
        expert(2, False)
        for c in range(chunks):
            wait_backo(c)
            up_copy(c).wait_recv()

            def close(i):
                total = combine_o(c, in_cols(i)) + near[c, :, in_cols(i)].astype(jnp.float32)
                mixed[:, out_cols(c, i)] = total.astype(jnp.bfloat16)

            loop(step // TILE, close)
        table_to(1, table, inner_dev).wait_send()
        for c in range(chunks):
            near_copy(c).wait_send()
            each_near(lambda other, i: goo_copy(c, other, i).wait_send())
            each_near(lambda other, i: back_copy(1, c, other, i).wait_send())
            for k in (0, 2, 3):
                each_all(lambda other, i: back_copy(k, c, other, i).wait_send())


def body(tokens, norm_gain, route_ids, route_gates, w_gate, w_up, w_down):
    rows, width = tokens.shape
    top = route_ids.shape[1]
    devices = lax.axis_size("ep")
    experts = devices
    ff = w_gate.shape[2]
    capacity = 3 * rows * top // (2 * experts)
    half, quarter = devices // 2, devices // 4
    count = half * capacity
    step = width // CHUNKS
    weights = (route_gates / jnp.sum(route_gates, axis=1, keepdims=True)).T
    table = jnp.concatenate([slot_index(route_ids, experts, capacity), weights])
    vmem = pl.BlockSpec(memory_space=pltpu.VMEM)
    hbm = pl.BlockSpec(memory_space=pl.ANY)
    bf16 = jnp.bfloat16
    dma = pltpu.SemaphoreType.DMA
    block = (CHUNKS, rows, step)
    each = dma((CHUNKS,))
    return pl.pallas_call(
        functools.partial(kernel, devices, capacity, top),
        out_shape=jax.ShapeDtypeStruct((rows, width), bf16),
        in_specs=[hbm, vmem, vmem, hbm, hbm, hbm],
        out_specs=vmem,
        scratch_shapes=[
            pltpu.VMEM(block, bf16),
            pltpu.VMEM(block, bf16),
            pltpu.VMEM(block, bf16),
            pltpu.VMEM(block, bf16),
            pltpu.VMEM((4,) + table.shape, jnp.float32),
            pltpu.VMEM((4, count, rows), bf16),
            pltpu.VMEM((4, rows, count), bf16),
            pltpu.VMEM((3, CHUNKS, count, step), bf16),
            pltpu.VMEM((CHUNKS, count // 2, step), bf16),
            pltpu.VMEM((4, CHUNKS, count // 2, step), bf16),
            pltpu.VMEM((count // 2, ff), bf16),
            pltpu.VMEM((width, ff), bf16),
            pltpu.VMEM((width, ff), bf16),
            pltpu.VMEM((ff, width), bf16),
            pltpu.VMEM((3, CHUNKS, count, step), bf16),
            pltpu.VMEM((CHUNKS, count // 2, step), bf16),
            pltpu.VMEM(block, bf16),
            pltpu.VMEM(block, bf16),
            dma((4,)), dma((4,)), dma((4,)),
            each, each, each, each, each, each,
            dma((3, CHUNKS, half)),
            dma((4, CHUNKS, quarter)),
            dma((CHUNKS, quarter)),
            dma((4, CHUNKS, quarter)),
            dma((3, CHUNKS, half)),
            dma((CHUNKS, quarter)),
            dma((4, CHUNKS)),
            dma((4, CHUNKS)),
            each, each, each, each, each, each,
        ],
        compiler_params=pltpu.CompilerParams(
            collective_id=0, has_side_effects=True, vmem_limit_bytes=VMEM_BYTES
        ),
    )(tokens, norm_gain[None, :], table, w_gate, w_up, w_down)


def solution(mesh):
    placed = (
        P(("grp", "ep"), None),
        P(),
        P(("grp", "ep"), None),
        P(("grp", "ep"), None),
        P("ep", None, None),
        P("ep", None, None),
        P("ep", None, None),
    )
    return jax.shard_map(
        body, mesh=mesh, in_specs=placed, out_specs=P(("grp", "ep"), None), check_vma=False
    )
```

```python
import functools

import jax
import jax.numpy as jnp
from jax import lax
from jax.experimental import pallas as pl
from jax.experimental.pallas import tpu as pltpu
from jax.sharding import PartitionSpec as P

EPS = 1e-06
CHUNKS = 4
TILE = 256
VMEM_BYTES = 66000000


def slot_index(route_ids, experts, capacity):
    rows, top = route_ids.shape
    hit = [route_ids[:, k : k + 1] == jnp.arange(experts, dtype=jnp.int32)[None, :] for k in range(top)]
    named = sum(h.astype(jnp.float32) for h in hit)
    before = (jnp.arange(rows)[:, None] > jnp.arange(rows)[None, :]).astype(jnp.bfloat16)
    ranked = jnp.dot(before, named.astype(jnp.bfloat16), preferred_element_type=jnp.float32)
    base = ranked + jnp.arange(experts, dtype=jnp.float32)[None, :] * capacity
    return jnp.stack([jnp.sum(jnp.where(h, base, 0.0), axis=1) for h in hit])


def dot32(a, b):
    return jnp.dot(a, b, preferred_element_type=jnp.float32)


def kernel(
    devices, capacity, top,
    tokens_hbm, gain, table, gate_hbm, up_hbm, down_hbm,
    mixed,
    normed, far, far_table, takes, highs, lows, packed, arrived, hidden, w_gate, w_up, w_down,
    outs, backs, partial, partial_in,
    weight_sems, table_sems, far_send, far_recv, own_sems, self_sems, go_send, go_recv,
    back_send, back_recv, part_send, part_recv,
):
    half = devices // 2
    chunks, rows, step = normed.shape
    count = half * capacity
    ff = w_gate.shape[1]
    me = lax.axis_index("ep")
    q = me % half
    base = me - q
    partner = (me + half) % devices
    first = base * capacity

    def peer_at(i):
        off = (half // 2 + i) % half + (half // 2 + i) // half
        return (q + off) % half

    barrier = pltpu.get_barrier_semaphore()

    def greet(i, carry):
        pl.semaphore_signal(barrier, inc=1, device_id={"ep": base + peer_at(i)})
        return carry

    token_load = pltpu.make_async_copy(tokens_hbm, mixed, weight_sems.at[3])
    token_load.start()
    lax.fori_loop(0, half - 1, greet, 0)
    pl.semaphore_signal(barrier, inc=1, device_id={"ep": partner})

    loads = [
        pltpu.make_async_copy(gate_hbm.at[0], w_gate, weight_sems.at[0]),
        pltpu.make_async_copy(up_hbm.at[0], w_up, weight_sems.at[1]),
        pltpu.make_async_copy(down_hbm.at[0], w_down, weight_sems.at[2]),
    ]
    token_load.wait()

    def norm(i, carry):
        at = pl.ds(pl.multiple_of(i * 64, 64), 64)
        floats = mixed[at, :].astype(jnp.float32)
        scale = lax.rsqrt(jnp.mean(floats * floats, axis=-1, keepdims=True) + EPS)
        value = (floats * scale * gain[...]).astype(jnp.bfloat16)
        for c in range(chunks):
            normed[c, at, :] = value[:, c * step : (c + 1) * step]
        return carry

    lax.fori_loop(0, rows // 64, norm, 0)
    pl.semaphore_wait(barrier, half)

    def remote(src, dst, send, recv, device):
        return pltpu.make_async_remote_copy(
            src_ref=src, dst_ref=dst, send_sem=send, recv_sem=recv, device_id={"ep": device}
        )

    def table_copy():
        return remote(table, far_table, table_sems.at[0], table_sems.at[1], partner)

    def far_copy(c):
        return remote(normed.at[c], far.at[c], far_send.at[c], far_recv.at[c], partner)

    def part_copy(c):
        return remote(partial.at[c], partial_in.at[c], part_send.at[c], part_recv.at[c], partner)

    def span(j):
        return pl.ds(pl.multiple_of(j * capacity, 16), capacity)

    def go_copy(s, c, peer, slot):
        return remote(
            packed.at[s, c, span(peer)], arrived.at[s, c, span(q)],
            go_send.at[s, c, slot], go_recv.at[s, c, q], base + peer,
        )

    def back_copy(s, c, peer, slot):
        return remote(
            outs.at[s, c, span(peer)], backs.at[s, c, span(q)],
            back_send.at[s, c, slot], back_recv.at[s, c, q], base + peer,
        )

    def go_arrival(s, c, peer):
        return remote(
            packed.at[s, c, span(peer)], arrived.at[s, c, span(peer)],
            go_send.at[s, c, 0], go_recv.at[s, c, peer], base + peer,
        )

    def back_arrival(s, c, peer):
        return remote(
            outs.at[s, c, span(peer)], backs.at[s, c, span(peer)],
            back_send.at[s, c, 0], back_recv.at[s, c, peer], base + peer,
        )

    def go_self(s, c):
        return pltpu.make_async_copy(packed.at[s, c, span(q)], arrived.at[s, c, span(q)], own_sems.at[s, c])

    def back_self(s, c):
        return pltpu.make_async_copy(outs.at[s, c, span(q)], backs.at[s, c, span(q)], self_sems.at[s, c])

    def each_peer(act):
        def one(i, carry):
            act(peer_at(i), i)
            return carry

        lax.fori_loop(0, half - 1, one, 0)

    def matrices(s, source):
        width = 128

        def one(i, carry):
            at = pl.multiple_of(i * width, width)
            slots = (first + at + lax.broadcasted_iota(jnp.int32, (width, rows), 0)).astype(jnp.float32)
            taken = jnp.zeros((width, rows), jnp.float32)
            total = jnp.zeros((width, rows), jnp.float32)
            for k in range(top):
                hit = source[k : k + 1, :] == slots
                taken = taken + jnp.where(hit, 1.0, 0.0)
                total = total + jnp.where(hit, source[top + k : top + k + 1, :], 0.0)
            takes[s, pl.ds(at, width), :] = taken.astype(jnp.bfloat16)
            turned = total.T
            high = turned.astype(jnp.bfloat16)
            highs[s, :, pl.ds(at, width)] = high
            lows[s, :, pl.ds(at, width)] = (turned - high.astype(jnp.float32)).astype(jnp.bfloat16)
            return carry

        lax.fori_loop(0, count // width, one, 0)

    def tiles(act):
        def one(i, carry):
            act(pl.ds(pl.multiple_of(i * TILE, TILE), TILE))
            return carry

        lax.fori_loop(0, step // TILE, one, 0)

    def pack(s, c, source):
        def one(cols):
            packed[s, c, :, cols] = dot32(takes[s], source[c, :, cols]).astype(jnp.bfloat16)

        tiles(one)
        each_peer(lambda peer, i: go_copy(s, c, peer, i).start())
        go_self(s, c).start()

    def wait_go(s, c):
        each_peer(lambda peer, i: go_arrival(s, c, peer).wait_recv())
        go_self(s, c).wait()

    def expert_hidden(s):
        def one(i, carry):
            cols = pl.ds(pl.multiple_of(i * TILE, TILE), TILE)
            gate_pre = dot32(arrived[s, 0], w_gate[0:step, cols])
            up_pre = dot32(arrived[s, 0], w_up[0:step, cols])
            for c in range(1, chunks):
                gate_pre += dot32(arrived[s, c], w_gate[c * step : (c + 1) * step, cols])
                up_pre += dot32(arrived[s, c], w_up[c * step : (c + 1) * step, cols])
            hidden[s, :, cols] = (gate_pre / (1.0 + jnp.exp(-gate_pre)) * up_pre).astype(jnp.bfloat16)
            return carry

        lax.fori_loop(0, ff // TILE, one, 0)

    def expert_out(s, c):
        def one(i, carry):
            at = pl.multiple_of(i * TILE, TILE)
            cols = pl.ds(pl.multiple_of(c * step + at, TILE), TILE)
            outs[s, c, :, pl.ds(at, TILE)] = dot32(hidden[s], w_down[:, cols]).astype(jnp.bfloat16)
            return carry

        lax.fori_loop(0, step // TILE, one, 0)

    def send_back(s, c):
        each_peer(lambda peer, i: back_copy(s, c, peer, i).start())
        back_self(s, c).start()

    def wait_back(s, c):
        each_peer(lambda peer, i: back_arrival(s, c, peer).wait_recv())
        back_self(s, c).wait()

    table_copy().start()
    far_copy(0).start()
    for load in loads:
        load.start()
    matrices(0, table)
    for c in range(chunks):
        pack(0, c, normed)
        if c + 1 < chunks:
            far_copy(c + 1).start()
    table_copy().wait()
    matrices(1, far_table)
    for c in range(chunks):
        far_copy(c).wait_recv()
        pack(1, c, far)
        if c == chunks - 2:
            for s_c in range(chunks):
                wait_go(0, s_c)
            for load in loads:
                load.wait()
            expert_hidden(0)
            for d in range(chunks):
                expert_out(0, d)
    for c in range(chunks):
        wait_go(1, c)
    for c in range(1):
        send_back(0, c)
    expert_hidden(1)
    for c in range(chunks):
        expert_out(1, c)
        send_back(1, c)
    for c in range(chunks):
        wait_back(1, c)

        def merge(cols):
            back = backs[1, c, :, cols]
            partial[c, :, cols] = (dot32(highs[1], back) + dot32(lows[1], back)).astype(jnp.bfloat16)

        tiles(merge)
        part_copy(c).start()
        if c >= 1:
            send_back(0, c)
    for c in range(chunks):
        wait_back(0, c)
        part_copy(c).wait_recv()

        def close(i, carry):
            at = pl.multiple_of(i * TILE, TILE)
            cols = pl.ds(at, TILE)
            back = backs[0, c, :, cols]
            total = dot32(highs[0], back) + dot32(lows[0], back) + partial_in[c, :, cols].astype(jnp.float32)
            mixed[:, pl.ds(pl.multiple_of(c * step + at, TILE), TILE)] = total.astype(jnp.bfloat16)
            return carry

        lax.fori_loop(0, step // TILE, close, 0)
    for c in range(chunks):
        far_copy(c).wait_send()
        part_copy(c).wait_send()
        for s in range(2):
            each_peer(lambda peer, i: go_copy(s, c, peer, i).wait_send())
            each_peer(lambda peer, i: back_copy(s, c, peer, i).wait_send())


def body(tokens, norm_gain, route_ids, route_gates, w_gate, w_up, w_down):
    rows, width = tokens.shape
    top = route_ids.shape[1]
    devices = lax.axis_size("ep")
    experts = devices
    ff = w_gate.shape[2]
    capacity = 3 * rows * top // (2 * experts)
    half = devices // 2
    count = half * capacity
    step = width // CHUNKS
    weights = (route_gates / jnp.sum(route_gates, axis=1, keepdims=True)).T
    table = jnp.concatenate([slot_index(route_ids, experts, capacity), weights])
    vmem = pl.BlockSpec(memory_space=pltpu.VMEM)
    hbm = pl.BlockSpec(memory_space=pl.ANY)
    bf16 = jnp.bfloat16
    dma = pltpu.SemaphoreType.DMA
    return pl.pallas_call(
        functools.partial(kernel, devices, capacity, top),
        out_shape=jax.ShapeDtypeStruct((rows, width), bf16),
        in_specs=[hbm, vmem, vmem, hbm, hbm, hbm],
        out_specs=vmem,
        scratch_shapes=[
            pltpu.VMEM((CHUNKS, rows, step), bf16),
            pltpu.VMEM((CHUNKS, rows, step), bf16),
            pltpu.VMEM(table.shape, jnp.float32),
            pltpu.VMEM((2, count, rows), bf16),
            pltpu.VMEM((2, rows, count), bf16),
            pltpu.VMEM((2, rows, count), bf16),
            pltpu.VMEM((2, CHUNKS, count, step), bf16),
            pltpu.VMEM((2, CHUNKS, count, step), bf16),
            pltpu.VMEM((2, count, ff), bf16),
            pltpu.VMEM((width, ff), bf16),
            pltpu.VMEM((width, ff), bf16),
            pltpu.VMEM((ff, width), bf16),
            pltpu.VMEM((2, CHUNKS, count, step), bf16),
            pltpu.VMEM((2, CHUNKS, count, step), bf16),
            pltpu.VMEM((CHUNKS, rows, step), bf16),
            pltpu.VMEM((CHUNKS, rows, step), bf16),
            dma((4,)),
            dma((2,)),
            dma((CHUNKS,)),
            dma((CHUNKS,)),
            dma((2, CHUNKS)),
            dma((2, CHUNKS)),
            dma((2, CHUNKS, half)),
            dma((2, CHUNKS, half)),
            dma((2, CHUNKS, half)),
            dma((2, CHUNKS, half)),
            dma((CHUNKS,)),
            dma((CHUNKS,)),
        ],
        compiler_params=pltpu.CompilerParams(
            collective_id=0, has_side_effects=True, vmem_limit_bytes=VMEM_BYTES
        ),
    )(tokens, norm_gain[None, :], table, w_gate, w_up, w_down)


def solution(mesh):
    placed = (
        P(("grp", "ep"), None),
        P(),
        P(("grp", "ep"), None),
        P(("grp", "ep"), None),
        P("ep", None, None),
        P("ep", None, None),
        P("ep", None, None),
    )
    return jax.shard_map(
        body, mesh=mesh, in_specs=placed, out_specs=P(("grp", "ep"), None), check_vma=False
    )
```
